32 devices in a mesh: tp: 16 (over z, y, x), dp: 2 (over core).
Axes of the slice: x: 2, y: 2, z: 4, core: 2. Of those that a mesh axis runs over, the one named last changes fastest.
Arguments:
- tokens: bfloat16 [64, 4096], P(None, 'dp'), may hold values from -6 to 6
- lengths: int32 [64], P('dp'), may hold values from 1 to 4096, 65536 in all
- norm_gain: float32 [2, 4096], P(None, 'dp'), may hold values from 0.1 to 1.9
- w_in: bfloat16 [2, 4096, 2048], P(None, 'dp', 'tp'), may hold values from -0.09375 to 0.09375
- log_step: float32 [2, 128], P(None, 'tp'), may hold values from -4.6 to -0.7
- eig_re: float32 [2, 128, 64], P(None, 'tp'), may hold values from -2 to -0.05
- eig_im: float32 [2, 128, 64], P(None, 'tp'), may hold values from 0 to 8
- in_mat: float32 [2, 2, 128, 64, 16], P(None, None, 'tp'), may hold values from -2.5 to 2.5
- output_matrices: float32 [2, 2, 128, 16, 64], P(None, None, 'tp'), may hold values from -1.25 to 1.25
- skip: float32 [2, 2048], P(None, 'tp'), may hold values from -4 to 4
- w_glu: bfloat16 [2, 2048, 4096], P(None, 'tp', 'dp'), may hold values from -0.375 to 0.375
- w_gate: bfloat16 [2, 2048, 4096], P(None, 'tp', 'dp'), may hold values from -0.125 to 0.125
- state: float32 [2, 2, 64, 8192], P(None, None, 'dp', 'tp'), may hold values from -6 to 6
Outputs:
- mixed: bfloat16 [64, 4096], P(None, 'dp')
- new_state: float32 [2, 2, 64, 8192], P(None, None, 'dp', 'tp')
The draws below stay inside these ranges and needn't reach their ends.
Inputs may be any that keep to these rules, and one draw needn't show every extreme that they name: `lengths`: each sequence's number of past positions; the largest is exactly 4096 and all add up to 65536.
All inputs are finite; a program needn't handle non-finite values.
Results may differ from the reference program's by a relative error of at most 0.0095.
Values may be sent and summed in bfloat16 or wider, within the bound.
A program may use at most 64 MiB of HBM per device.

```python
import math
import jax
import jax.numpy as jnp
import numpy as np
from jax import lax

D = 4096
GROUPS = 128
GROUP = 16
STATES = 64
S5W = 2048
LAYERS = 2
BATCH = 64
LEN_MAX = 4096
LEN_MEAN = 1024
BLOCK_LEN = 256


def spiked(array, stream_key, source, target, shards_of, factor):
    owner, partner = [(jnp.arange(array.shape[dim]) // (array.shape[dim] // shards_of)).reshape([-1 if axis == dim else 1 for axis in range(array.ndim)]) for dim in (source, target)]
    chosen = jax.random.permutation(stream_key, shards_of)[partner]
    strong = (owner == chosen) | (owner == (partner + shards_of // 2) % shards_of)
    return jnp.where(strong, factor * array, array)


def block_levels(own_key, dims, pieces, low, top_value):
    def one(position, shards_of):
        draws = jax.random.uniform(jax.random.fold_in(jax.random.fold_in(own_key, 6), position), (shards_of,), jnp.float32, low / len(pieces), top_value / len(pieces))
        return jnp.repeat(jnp.exp(draws), dims[position] // shards_of).reshape((-1,) + (1,) * (len(dims) - position - 1))

    level = one(*pieces[0])
    for cut in pieces[1:]:
        level = level * one(*cut)
    return level


def profile(number_of, total, reach, lean):
    loads = [(1 << 20) // math.isqrt(grade ** lean) + 1 for grade in range(2, number_of + 1)]
    rest, holding = total - reach - (number_of - 1), [1] * (number_of - 1)
    while rest > 0:
        candidates = [i for i in range(number_of - 1) if holding[i] < reach]
        mass, remaining = sum([loads[i] for i in candidates]), rest
        for i in candidates:
            extra = min(reach - holding[i], max(1, remaining * loads[i] // mass), rest)
            holding[i] = holding[i] + extra
            rest = rest - extra
    return np.array([reach] + holding)


def ragged(rng, amount, total, reach, skew):
    if amount == 2:
        one = jax.random.randint(rng, (), max(1, total - reach), min(reach, total - 1) + 1)
        return jnp.stack([one, total - one])
    sizes = jnp.asarray(profile(amount, total, reach, skew), jnp.int32)
    couples = (amount - 1) // 2
    giver, sink = sizes[1:1 + 2 * couples:2], sizes[2:2 + 2 * couples:2]
    slack = jnp.minimum(giver - 1, reach - sink)
    moved = jax.random.randint(jax.random.fold_in(rng, 1), (couples,), 0, 1 << 20) % (slack + 1)
    sizes = sizes.at[1:1 + 2 * couples:2].set(giver - moved).at[2:2 + 2 * couples:2].set(sink + moved)
    return sizes[jax.random.permutation(jax.random.fold_in(rng, 2), amount)]


def scatter_about(rng, extent, spread, limit, split=(), kind=jnp.bfloat16):
    result = spread * jax.random.normal(rng, extent, jnp.float32)
    if split:
        result = result * block_levels(rng, extent, split, -0.22, 0.18)
    return jnp.clip(result, -limit, limit).astype(kind)


def noise_with(key, dims, deviation, most, pieces, heavy, kind=jnp.bfloat16):
    entries = deviation * jax.random.normal(key, dims, jnp.float32)
    if pieces:
        entries = entries * block_levels(key, dims, pieces, -0.22, 0.18)
    return jnp.clip(spiked(entries, jax.random.fold_in(key, 3), *heavy), -most, most).astype(kind)


def setup_inputs(seed: int = 0) -> dict:
    arg_keys = jax.random.split(jax.random.key(seed), 14)
    return {
        "tokens": scatter_about(arg_keys[0], (BATCH, D), 1.0, 6.0, ((1, 2),)),
        "lengths": ragged(arg_keys[1], BATCH, BATCH * LEN_MEAN, LEN_MAX, 2).astype(jnp.int32),
        "norm_gain": jnp.clip(1.0 + 0.18 * jax.random.normal(arg_keys[2], (LAYERS, D), jnp.float32), 0.1, 1.9),
        "w_in": scatter_about(arg_keys[3], (LAYERS, D, S5W), D ** -0.5, 0.09375, ((1, 2), (2, 16))),
        "log_step": jnp.clip(-4.6 + 3.8999999 * jax.random.uniform(arg_keys[4], (LAYERS, GROUPS), jnp.float32) ** block_levels(arg_keys[4], (LAYERS, GROUPS), ((1, 16),), -0.2, 0.2), -4.6, -0.7),
        "eig_re": jnp.clip(-2.0 + 1.95 * jax.random.uniform(arg_keys[5], (LAYERS, GROUPS, STATES), jnp.float32) ** block_levels(arg_keys[5], (LAYERS, GROUPS, STATES), ((1, 16),), -0.2, 0.2), -2.0, -0.05),
        "eig_im": jnp.clip(8.0 * jax.random.uniform(arg_keys[6], (LAYERS, GROUPS, STATES), jnp.float32) ** block_levels(arg_keys[6], (LAYERS, GROUPS, STATES), ((1, 16),), -0.2, 0.2), 0.0, 8.0),
        "in_mat": scatter_about(arg_keys[7], (LAYERS, 2, GROUPS, STATES, GROUP), 0.177, 2.5, ((2, 16),), jnp.float32),
        "output_matrices": scatter_about(arg_keys[8], (LAYERS, 2, GROUPS, GROUP, STATES), 0.088, 1.25, ((2, 16),), jnp.float32),
        "skip": scatter_about(arg_keys[9], (LAYERS, S5W), 1.0, 4.0, ((1, 16),), jnp.float32),
        "w_glu": noise_with(arg_keys[10], (LAYERS, S5W, D), (S5W // 4) ** -0.5, 0.375, ((1, 16), (2, 2)), (1, 2, 16, 2.0)),
        "w_gate": scatter_about(arg_keys[11], (LAYERS, S5W, D), S5W ** -0.5, 0.125, ((1, 16), (2, 2))),
        "state": scatter_about(arg_keys[12], (LAYERS, 2, BATCH, GROUPS * STATES), 0.5, 6.0, ((2, 2), (3, 16)), jnp.float32),
    }


NORM_EPS = 1e-06
FULL_PRECISION = lax.Precision.HIGHEST

def position_factor(lengths):
    blocks = (lengths // BLOCK_LEN).astype(jnp.float32)
    return 2.0 / (1.0 + blocks * (4.0 * BLOCK_LEN / LEN_MAX))

def recurrent_step(driven_state, state_pair, factor, log_step, eig_re, eig_im, in_mat, output_matrices, skip):
    step_size = jnp.exp(log_step)[None, :, None] * factor[:, None, None]
    magnitude = jnp.exp(eig_re[None] * step_size)
    turned = eig_im[None] * step_size
    decay_re = magnitude * jnp.cos(turned)
    decay_im = magnitude * jnp.sin(turned)
    modulus = eig_re * eig_re + eig_im * eig_im
    weight_re = ((decay_re - 1.0) * eig_re + decay_im * eig_im) / modulus
    weight_im = (decay_im * eig_re - (decay_re - 1.0) * eig_im) / modulus
    drive_re = jnp.einsum('bgc,gpc->bgp', driven_state, in_mat[0], precision=FULL_PRECISION)
    drive_im = jnp.einsum('bgc,gpc->bgp', driven_state, in_mat[1], precision=FULL_PRECISION)
    state_real = decay_re * state_pair[0] - decay_im * state_pair[1] + weight_re * drive_re - weight_im * drive_im
    state_imaginary = decay_re * state_pair[1] + decay_im * state_pair[0] + weight_re * drive_im + weight_im * drive_re
    readout_value = jnp.einsum('szv,zuv->szu', state_real, output_matrices[0], precision=FULL_PRECISION) - jnp.einsum('szv,zuv->szu', state_imaginary, output_matrices[1], precision=FULL_PRECISION) + skip * driven_state
    return (jax.nn.gelu(readout_value), state_real, state_imaginary)

def reference(tokens, lengths, norm_gain, w_in, log_step, eig_re, eig_im, in_mat, output_matrices, skip, w_glu, w_gate, state):
    factor = position_factor(lengths)
    current = tokens.astype(jnp.float32)
    rounded = tokens
    new_states = []
    for layer_index in range(LAYERS):
        squares = lax.optimization_barrier(jnp.sum(current * current, axis=1))
        scaled = (current * norm_gain[layer_index]).astype(jnp.bfloat16)
        partial_value = jnp.dot(scaled, w_in[layer_index], preferred_element_type=jnp.float32)
        driven_state = (partial_value * lax.rsqrt(squares / D + NORM_EPS)[:, None]).astype(jnp.bfloat16)
        driven_state = driven_state.astype(jnp.float32).reshape(BATCH, GROUPS, GROUP)
        state_pair = state[layer_index].reshape(2, BATCH, GROUPS, STATES)
        readout_value, state_real, state_imaginary = recurrent_step(driven_state, state_pair, factor, log_step[layer_index], eig_re[layer_index], eig_im[layer_index], in_mat[layer_index], output_matrices[layer_index], skip[layer_index].reshape(GROUPS, GROUP))
        readout_value = readout_value.reshape(BATCH, GROUPS * GROUP).astype(jnp.bfloat16)
        new_states.append(jnp.stack([state_real, state_imaginary]).reshape(2, BATCH, GROUPS * STATES))
        linear = jnp.dot(readout_value, w_glu[layer_index], preferred_element_type=jnp.float32)
        gate_sum = jnp.dot(readout_value, w_gate[layer_index], preferred_element_type=jnp.float32)
        rounded = (current + linear * jax.nn.sigmoid(gate_sum)).astype(jnp.bfloat16)
        current = rounded.astype(jnp.float32)
    return (rounded, jnp.stack(new_states))
```

```python
import functools

import jax
import jax.numpy as jnp
from jax import lax
from jax.experimental import pallas as pl
from jax.experimental.pallas import tpu as pltpu
from jax.sharding import PartitionSpec as P

D = 4096
GROUP = 16
STATES = 64
LAYERS = 2
LEN_MAX = 4096
BLOCK_LEN = 256


NORM_EPS = 1e-06
FULL_PRECISION = lax.Precision.HIGHEST


def position_factor(lengths):
    blocks = (lengths // BLOCK_LEN).astype(jnp.float32)
    return 2.0 / (1.0 + blocks * (4.0 * BLOCK_LEN / LEN_MAX))


def recurrent_step(
    driven_state, state_pair, factor, log_step, eig_re, eig_im, in_mat, output_matrices, skip
):
    step_size = jnp.exp(log_step)[None, :, None] * factor[:, None, None]
    magnitude = jnp.exp(eig_re[None] * step_size)
    turned = eig_im[None] * step_size
    decay_re = magnitude * jnp.cos(turned)
    decay_im = magnitude * jnp.sin(turned)
    modulus = eig_re * eig_re + eig_im * eig_im
    weight_re = ((decay_re - 1.0) * eig_re + decay_im * eig_im) / modulus
    weight_im = (decay_im * eig_re - (decay_re - 1.0) * eig_im) / modulus
    drive_re = jnp.einsum("bgc,gpc->bgp", driven_state, in_mat[0], precision=FULL_PRECISION)
    drive_im = jnp.einsum("bgc,gpc->bgp", driven_state, in_mat[1], precision=FULL_PRECISION)
    state_real = (
        decay_re * state_pair[0]
        - decay_im * state_pair[1]
        + weight_re * drive_re
        - weight_im * drive_im
    )
    state_imaginary = (
        decay_re * state_pair[1]
        + decay_im * state_pair[0]
        + weight_re * drive_im
        + weight_im * drive_re
    )
    readout_value = (
        jnp.einsum("szv,zuv->szu", state_real, output_matrices[0], precision=FULL_PRECISION)
        - jnp.einsum("szv,zuv->szu", state_imaginary, output_matrices[1], precision=FULL_PRECISION)
        + skip * driven_state
    )
    return (jax.nn.gelu(readout_value), state_real, state_imaginary)


def body(
    tokens,
    lengths,
    norm_gain,
    w_in,
    log_step,
    eig_re,
    eig_im,
    in_mat,
    output_matrices,
    skip,
    w_glu,
    w_gate,
    state,
):
    factor = position_factor(lengths)
    current = tokens.astype(jnp.float32)
    rounded = tokens
    new_states = []
    for layer_index in range(LAYERS):
        squares = jnp.sum(current * current, axis=1)
        scaled = (current * norm_gain[layer_index]).astype(jnp.bfloat16)
        partial_value = jnp.dot(scaled, w_in[layer_index], preferred_element_type=jnp.float32)
        summed, total_squares = (
            lax.psum_scatter(partial_value, "dp", scatter_dimension=0, tiled=True),
            lax.psum_scatter(squares, "dp", scatter_dimension=0, tiled=True),
        )
        driven_state = (summed * lax.rsqrt(total_squares / D + NORM_EPS)[:, None]).astype(
            jnp.bfloat16
        )
        own_seqs = driven_state.shape[0]
        group_count = log_step.shape[1]
        driven_state = driven_state.astype(jnp.float32).reshape(own_seqs, group_count, GROUP)
        state_pair = state[layer_index].reshape(2, own_seqs, group_count, STATES)
        readout_value, state_real, state_imaginary = recurrent_step(
            driven_state,
            state_pair,
            factor,
            log_step[layer_index],
            eig_re[layer_index],
            eig_im[layer_index],
            in_mat[layer_index],
            output_matrices[layer_index],
            skip[layer_index].reshape(group_count, GROUP),
        )
        readout_value = readout_value.reshape(own_seqs, group_count * GROUP).astype(jnp.bfloat16)
        new_states.append(
            jnp.stack([state_real, state_imaginary]).reshape(2, own_seqs, group_count * STATES)
        )
        glu_weight = w_glu[layer_index]
        gate_matrix = w_gate[layer_index]
        piece = lax.all_gather(readout_value, "dp", axis=0, tiled=True)
        combined_terms = jnp.stack(
            [
                jnp.dot(piece, glu_weight, preferred_element_type=jnp.float32),
                jnp.dot(piece, gate_matrix, preferred_element_type=jnp.float32),
            ]
        )
        totals = lax.psum(combined_terms, "tp")
        rounded = (current + totals[0] * jax.nn.sigmoid(totals[1])).astype(jnp.bfloat16)
        current = rounded.astype(jnp.float32)
    return (rounded, jnp.stack(new_states))


PLANE = 4
HALF = 2
LANES = 128
MESH = pl.DeviceIdType.MESH


def kernel(
    tp,
    tokens_ref,
    lengths_ref,
    gain_ref,
    w_in_ref,
    params_ref,
    in_ref,
    out_mat_ref,
    skip_ref,
    glu_ref,
    gate_ref,
    state_ref,
    mixed_ref,
    new_state_ref,
    chunks,
    swap_out,
    swap_in,
    readouts,
    terms,
    plane_in,
    column_out,
    column_in,
    coef,
    in_big,
    out_big,
    swap_sem,
    readout_sem,
    plane_sem,
    column_sem,
    gather_col_sem,
    gather_plane_sem,
):
    depth = tp // PLANE
    t = lax.axis_index("tp")
    d = lax.axis_index("dp")
    other = 1 - d
    z, place = t // PLANE, t % PLANE
    py, px = place // HALF, place % HALF

    def mate(q):
        return ((py + q // HALF) % HALF) * HALF + (px + q % HALF) % HALF

    def at(zz, pp):
        return {"tp": zz * PLANE + pp}

    mates = range(1, PLANE)
    columns = range(1, depth)

    barrier = pltpu.get_barrier_semaphore()
    pl.semaphore_signal(barrier, inc=1, device_id={"dp": other}, device_id_type=MESH)
    for q in mates:
        pl.semaphore_signal(barrier, inc=1, device_id=at(z, mate(q)), device_id_type=MESH)
    for dz in columns:
        pl.semaphore_signal(
            barrier, inc=1, device_id=at((z + dz) % depth, place), device_id_type=MESH
        )

    rows, features = tokens_ref.shape
    own = rows // HALF
    span = state_ref.shape[3]
    channels = skip_ref.shape[1]
    blocks = (lengths_ref[...] // BLOCK_LEN).astype(jnp.float32)
    factor = 2.0 / (1.0 + blocks * (4.0 * BLOCK_LEN / LEN_MAX))

    def prepare(layer):
        re = params_ref[layer, 0:1, :]
        im = params_ref[layer, 1:2, :]
        step_size = jnp.exp(params_ref[layer, 2:3, :]) * factor
        magnitude = jnp.exp(re * step_size)
        turned = im * step_size
        decay_re = magnitude * jnp.cos(turned)
        decay_im = magnitude * jnp.sin(turned)
        modulus = re * re + im * im
        coef[layer, 0] = decay_re
        coef[layer, 1] = decay_im
        coef[layer, 2] = ((decay_re - 1.0) * re + decay_im * im) / modulus
        coef[layer, 3] = (decay_im * re - (decay_re - 1.0) * im) / modulus
        groups = channels // GROUP
        group_of_row = lax.broadcasted_iota(jnp.int32, (channels, 2 * span), 0) // GROUP
        group_of_col = (lax.broadcasted_iota(jnp.int32, (channels, 2 * span), 1) % span) // STATES
        inside = group_of_row == group_of_col
        in_big[layer] = jnp.where(inside, jnp.concatenate([in_ref[layer]] * groups, axis=0), 0.0)
        out_big[layer] = jnp.where(
            inside, jnp.concatenate([out_mat_ref[layer]] * groups, axis=0), 0.0
        )

    for c in range(tp):
        chunks[0, c] = tokens_ref[:, c * LANES : (c + 1) * LANES]
    prepare(0)
    pl.semaphore_wait(barrier, 1 + len(mates) + len(columns))

    started = []

    def send(src, dst, sems, index, device):
        copy = pltpu.make_async_remote_copy(
            src_ref=src,
            dst_ref=dst,
            send_sem=sems.at[(0,) + index],
            recv_sem=sems.at[(1,) + index],
            device_id=device,
            device_id_type=MESH,
        )
        copy.start()
        started.append(copy)
        return copy

    last = LAYERS - 1
    for layer in range(LAYERS):
        squares = jnp.zeros((rows, LANES), jnp.float32)
        scaled = []
        for c in range(tp):
            value = chunks[layer, c].astype(jnp.float32)
            squares = squares + value * value
            scaled.append(
                (value * gain_ref[layer : layer + 1, c * LANES : (c + 1) * LANES]).astype(
                    jnp.bfloat16
                )
            )
        partial_value = jnp.dot(
            jnp.concatenate(scaled, axis=1), w_in_ref[layer], preferred_element_type=jnp.float32
        )
        total = jnp.broadcast_to(jnp.sum(squares, axis=1, keepdims=True), (rows, LANES))
        for half in range(HALF):
            swap_out[layer, half, :, :LANES] = partial_value[half * own : (half + 1) * own]
            swap_out[layer, half, :, LANES:] = total[half * own : (half + 1) * own]
        swap = send(
            swap_out.at[layer, other], swap_in.at[layer], swap_sem, (layer,), {"dp": other}
        )
        swap.wait_recv()
        both = swap_out[layer, d] + swap_in[layer]
        driven = (both[:, :LANES] * lax.rsqrt(both[:, LANES:] / D + NORM_EPS)).astype(jnp.bfloat16)
        driven = driven.astype(jnp.float32)
        drive = jnp.dot(
            driven, in_big[layer], preferred_element_type=jnp.float32, precision=FULL_PRECISION
        )
        drive_re, drive_im = drive[:, :span], drive[:, span:]
        old_re, old_im = state_ref[layer, 0], state_ref[layer, 1]
        decay_re, decay_im = coef[layer, 0], coef[layer, 1]
        weight_re, weight_im = coef[layer, 2], coef[layer, 3]
        state_re = (
            decay_re * old_re - decay_im * old_im + weight_re * drive_re - weight_im * drive_im
        )
        state_im = (
            decay_re * old_im + decay_im * old_re + weight_re * drive_im + weight_im * drive_re
        )
        new_state_ref[layer, 0] = state_re
        new_state_ref[layer, 1] = state_im
        read = lax.dot_general(
            jnp.concatenate([state_re, -state_im], axis=1),
            out_big[layer],
            (((1,), (1,)), ((), ())),
            preferred_element_type=jnp.float32,
            precision=FULL_PRECISION,
        )
        read = jax.nn.gelu(read + skip_ref[layer : layer + 1, :] * driven)
        readouts[layer, d] = read.astype(jnp.bfloat16)
        swap = send(
            readouts.at[layer, d], readouts.at[layer, d], readout_sem, (layer,), {"dp": other}
        )
        swap.wait_recv()
        piece = jnp.concatenate([readouts[layer, half] for half in range(HALF)], axis=0)
        linear = jnp.dot(piece, glu_ref[layer], preferred_element_type=jnp.float32)
        gate = jnp.dot(piece, gate_ref[layer], preferred_element_type=jnp.float32)
        for c in range(tp):
            terms[layer, c, 0] = linear[:, c * LANES : (c + 1) * LANES].astype(jnp.bfloat16)
            terms[layer, c, 1] = gate[:, c * LANES : (c + 1) * LANES].astype(jnp.bfloat16)

        order = [dz for dz in range(depth - 1, 0, -1)] + [0]
        arrivals = {}
        for dz in order:
            target = (z + dz) % depth
            for q in mates:
                arrivals[q, dz] = send(
                    terms.at[layer, target * PLANE + mate(q)],
                    plane_in.at[layer, q - 1, dz],
                    plane_sem,
                    (layer, q - 1, dz),
                    at(z, mate(q)),
                )
        if layer < last:
            prepare(layer + 1)
        column = {}
        for dz in order:
            target = (z + dz) % depth
            for q in mates:
                arrivals[q, dz].wait_recv()
            value = terms[layer, target * PLANE + place].astype(jnp.float32)
            for q in mates:
                value = value + plane_in[layer, q - 1, dz].astype(jnp.float32)
            if dz == 0:
                summed = value
            else:
                column_out[layer, dz - 1] = value.astype(jnp.bfloat16)
                column[dz] = send(
                    column_out.at[layer, dz - 1],
                    column_in.at[layer, dz - 1],
                    column_sem,
                    (layer, dz - 1),
                    at(target, place),
                )
        for dz in columns:
            column[dz].wait_recv()
            summed = summed + column_in[layer, dz - 1].astype(jnp.float32)
        current = chunks[layer, t].astype(jnp.float32)
        mixed = current + summed[0] * jax.nn.sigmoid(summed[1])
        chunks[layer + 1, t] = mixed.astype(jnp.bfloat16)

        gathered = {}
        mine = chunks.at[layer + 1, t]
        for dz in columns:
            column[dz] = send(
                mine, mine, gather_col_sem, (layer, dz - 1), at((z + dz) % depth, place)
            )
        for q in mates:
            gathered[q, 0] = send(
                mine, mine, gather_plane_sem, (layer, q - 1, 0), at(z, mate(q))
            )
        for dz in columns:
            column[dz].wait_recv()
            passed = chunks.at[layer + 1, ((z + depth - dz) % depth) * PLANE + place]
            for q in mates:
                gathered[q, dz] = send(
                    passed, passed, gather_plane_sem, (layer, q - 1, dz), at(z, mate(q))
                )
        for key in gathered:
            gathered[key].wait_recv()
    for c in range(tp):
        mixed_ref[:, c * LANES : (c + 1) * LANES] = chunks[LAYERS, c]
    for copy in started:
        copy.wait_send()


def fused(
    tp,
    tokens,
    lengths,
    norm_gain,
    w_in,
    log_step,
    eig_re,
    eig_im,
    in_mat,
    output_matrices,
    skip,
    w_glu,
    w_gate,
    state,
):
    rows, features = tokens.shape
    own = rows // HALF
    groups = log_step.shape[1]
    span = groups * STATES
    channels = groups * GROUP
    depth = tp // PLANE
    steps = jnp.broadcast_to(log_step[:, :, None], eig_re.shape)
    params = jnp.stack([eig_re, eig_im, steps], axis=1).reshape(LAYERS, 3, span)
    in_rows = jnp.transpose(in_mat, (0, 4, 1, 2, 3)).reshape(LAYERS, GROUP, 2 * span)
    out_rows = jnp.transpose(output_matrices, (0, 3, 1, 2, 4)).reshape(LAYERS, GROUP, 2 * span)
    wire = jnp.bfloat16
    return tuple(
        pl.pallas_call(
            functools.partial(kernel, tp),
            out_shape=[
                jax.ShapeDtypeStruct(tokens.shape, jnp.bfloat16),
                jax.ShapeDtypeStruct(state.shape, jnp.float32),
            ],
            in_specs=[pl.BlockSpec(memory_space=pltpu.VMEM)] * 11,
            out_specs=[pl.BlockSpec(memory_space=pltpu.VMEM)] * 2,
            scratch_shapes=[
                pltpu.VMEM((LAYERS + 1, tp, rows, LANES), wire),
                pltpu.VMEM((LAYERS, HALF, own, 2 * LANES), jnp.float32),
                pltpu.VMEM((LAYERS, own, 2 * LANES), jnp.float32),
                pltpu.VMEM((LAYERS, HALF, own, channels), wire),
                pltpu.VMEM((LAYERS, tp, 2, rows, LANES), wire),
                pltpu.VMEM((LAYERS, PLANE - 1, depth, 2, rows, LANES), wire),
                pltpu.VMEM((LAYERS, depth - 1, 2, rows, LANES), wire),
                pltpu.VMEM((LAYERS, depth - 1, 2, rows, LANES), wire),
                pltpu.VMEM((LAYERS, 4, own, span), jnp.float32),
                pltpu.VMEM((LAYERS, channels, 2 * span), jnp.float32),
                pltpu.VMEM((LAYERS, channels, 2 * span), jnp.float32),
                pltpu.SemaphoreType.DMA((2, LAYERS)),
                pltpu.SemaphoreType.DMA((2, LAYERS)),
                pltpu.SemaphoreType.DMA((2, LAYERS, PLANE - 1, depth)),
                pltpu.SemaphoreType.DMA((2, LAYERS, depth - 1)),
                pltpu.SemaphoreType.DMA((2, LAYERS, depth - 1)),
                pltpu.SemaphoreType.DMA((2, LAYERS, PLANE - 1, depth)),
            ],
            compiler_params=pltpu.CompilerParams(
                collective_id=0, has_side_effects=True, vmem_limit_bytes=48 * 1024 * 1024
            ),
        )(
            tokens,
            lengths.reshape(own, 1),
            norm_gain,
            w_in,
            params,
            in_rows,
            out_rows,
            skip,
            w_glu,
            w_gate,
            state,
        )
    )


def dispatch(tp, dp, *args):
    tokens, skip, w_in = args[0], args[9], args[3]
    fits = (
        dp == HALF
        and tp % PLANE == 0
        and tp > PLANE
        and tokens.shape[1] == tp * LANES
        and skip.shape[1] == LANES
        and w_in.shape[2] == LANES
        and tokens.shape[0] % (16 * HALF) == 0
    )
    return fused(tp, *args) if fits else body(*args)


def solution(mesh):
    placed = (
        P(None, "dp"),
        P("dp"),
        P(None, "dp"),
        P(None, "dp", "tp"),
        P(None, "tp"),
        P(None, "tp", None),
        P(None, "tp", None),
        P(None, None, "tp", None, None),
        P(None, None, "tp", None, None),
        P(None, "tp"),
        P(None, "tp", "dp"),
        P(None, "tp", "dp"),
        P(None, None, "dp", "tp"),
    )
    return jax.shard_map(
        functools.partial(dispatch, mesh.shape["tp"], mesh.shape["dp"]),
        mesh=mesh,
        in_specs=placed,
        out_specs=(P(None, "dp"), P(None, None, "dp", "tp")),
        check_vma=False,
    )
```
